32 devices in a mesh: grp: 2 (over x), tp: 4 (over y, core), dp: 4 (over z).
Axes of the slice: x: 2, y: 2, z: 4, core: 2. Of those that a mesh axis runs over, the one named last changes fastest.
Arguments:
- tokens: bfloat16 [512, 2048], P(('grp', 'tp'), 'dp'), parts along dimension 0, may hold values from -25 to 25
- state: float32 [2, 512, 16, 128, 128], P(None, ('grp', 'dp'), 'tp'), parts along dimension 1, may hold values from -1 to 1
- lengths: int32 [512], P(('grp', 'dp')), parts along dimension 0, may hold values from 1 to 4096, 131072 in all
- norm_gain: bfloat16 [2, 2048], P(None, 'dp'), may hold values from 0.099609375 to 1.8984375
- w_query: bfloat16 [2, 2048, 2048], P(None, 'dp', 'tp'), may hold values from -0.125 to 0.125
- w_forget: bfloat16 [2, 2048, 2048], P(None, 'dp', 'tp'), may hold values from -0.125 to 0.125
- w_input: bfloat16 [2, 2048, 2048], P(None, 'dp', 'tp'), may hold values from -0.125 to 0.125
- w_gate: bfloat16 [2, 2048, 2048], P(None, 'dp', 'tp'), may hold values from -0.125 to 0.125
- w_out: bfloat16 [2, 2048, 2048], P(None, 'tp', 'dp'), may hold values from -0.125 to 0.125
- bound_logit: float32 [2, 2048], P(None, 'tp'), may hold values from -3 to 5
- pace: float32 [2, 2048], P(None, 'tp'), may hold values from 0.6 to 2
- head_gain: float32 [2, 128], replicated, may hold values from 0.4 to 2.5
Outputs:
- mixed: float32 [512, 2048], P(('grp', 'tp'), 'dp'), parts along dimension 0
- new_state: float32 [2, 512, 16, 128, 128], P(None, ('grp', 'dp'), 'tp'), parts along dimension 1
The draws below stay inside these ranges and needn't reach their ends.
There are 2 independent parts, one for each index of `grp`. The reference program is written for one: setup_inputs(seed, part) draws one part's arguments, and reference() takes and returns one part's arrays. A program takes and returns all parts, laid end to end along the dimension named above; an argument that names none is the same for every part. Nothing has to cross between parts.
All inputs are finite; a program needn't handle non-finite values. No bound on the sum of `lengths` on one device may be relied on, other than what follows from the above.
Results may differ from the reference program's by a relative error of at most 0.0083.
Values may be sent and summed in bfloat16 or wider, within the bound.
A program may use at most 192 MiB of HBM per device.

```python
import math
import jax
import jax.numpy as jnp
import numpy as np
from jax import lax

D = 2048
HEADS = 16
HEAD = 128
KW = 2048
BATCH = 256
LENGTH_MEAN = 512
LONGEST = 4096


def draw_tokens(key, part):
    first, second = jax.random.split(jax.random.fold_in(key, 11), 2)
    level = jnp.exp(jax.random.uniform(second, (16,), jnp.float32, -1.2, 0.0))
    level = jnp.repeat(level, D // 16)
    base = jax.random.normal(first, (BATCH, D), jnp.float32)
    return jnp.clip(base * level[None, :], -25.0, 25.0).astype(jnp.bfloat16)


def draw_bound_logit(key, part):
    first, second, third = jax.random.split(jax.random.fold_in(key, 23), 3)
    quick = jax.random.bernoulli(first, 0.5, (2, HEADS))
    quick = jnp.repeat(quick, HEAD, axis=1)
    fast_values = jax.random.uniform(second, (2, KW), jnp.float32, -3.0, -1.0)
    slow_values = jax.random.uniform(third, (2, KW), jnp.float32, 2.0, 5.0)
    return jnp.where(quick, fast_values, slow_values).astype(jnp.float32)


def levels(stream_key, dims, shards, low, top_value):
    factor_of = 1.0
    for dim, blocks in shards:
        heights = jax.random.uniform(jax.random.fold_in(jax.random.fold_in(stream_key, 6), dim), (blocks,), jnp.float32, low / len(shards), top_value / len(shards))
        factor_of = factor_of * jnp.repeat(jnp.exp(heights), dims[dim] // blocks).reshape((-1,) + (1,) * (len(dims) - 1 - dim))
    return factor_of


def length_profile(amount, total, bound, lean):
    weights = [(1 << 20) // math.isqrt(standing ** lean) + 1 for standing in range(2, amount + 1)]
    rest, holding = total - bound - (amount - 1), [1] * (amount - 1)
    while rest > 0:
        candidates = [i for i in range(amount - 1) if holding[i] < bound]
        pool, remaining = sum([weights[i] for i in candidates]), rest
        for i in candidates:
            more = min(bound - holding[i], max(1, remaining * weights[i] // pool), rest)
            holding[i] = holding[i] + more
            rest = rest - more
    return np.array([bound] + holding)


def ragged_sizes(rng, amount, total, bound, skew):
    if amount == 2:
        one = jax.random.randint(rng, (), max(1, total - bound), min(bound, total - 1) + 1)
        return jnp.stack([one, total - one])
    sizes = jnp.asarray(length_profile(amount, total, bound, skew), jnp.int32)
    pairs = (amount - 1) // 2
    giver, taker = sizes[1:1 + 2 * pairs:2], sizes[2:2 + 2 * pairs:2]
    slack = jnp.minimum(giver - 1, bound - taker)
    shifted = jax.random.randint(jax.random.fold_in(rng, 1), (pairs,), 0, 1 << 20) % (slack + 1)
    sizes = sizes.at[1:1 + 2 * pairs:2].set(giver - shifted).at[2:2 + 2 * pairs:2].set(taker + shifted)
    return sizes[jax.random.permutation(jax.random.fold_in(rng, 2), amount)]


def noise(own_key, shape, deviation, most, cuts=(), kind=jnp.bfloat16):
    loudness = levels(own_key, shape, cuts, -0.22, 0.18) if cuts else 1.0
    entries = jax.random.normal(own_key, shape, jnp.float32) * deviation * loudness
    return jnp.minimum(jnp.maximum(entries, -most), most).astype(kind)


def setup_inputs(seed: int = 0, part: int = 0) -> dict:
    streams_of = jax.random.split(jax.random.key(seed), 13)
    own_keys = jax.random.split(jax.random.fold_in(streams_of[12], part), 13)
    tokens = draw_tokens(jax.random.fold_in(jax.random.fold_in(streams_of[12], part), 71), part)
    state = noise(own_keys[1], (2, BATCH, HEADS, HEAD, HEAD), 0.15, 1.0, ((1, 4), (2, 4)), jnp.float32)
    lengths = ragged_sizes(own_keys[2], BATCH, BATCH * LENGTH_MEAN, LONGEST, 2).astype(jnp.int32)
    norm_gain = jnp.clip(1.0 + 0.18 * jax.random.normal(streams_of[3], (2, D), jnp.float32), 0.099609375, 1.8984375).astype(jnp.bfloat16)
    w_query = noise(streams_of[4], (2, D, KW), D ** -0.5, 0.125, ((1, 4), (2, 4)))
    w_forget = noise(streams_of[5], (2, D, KW), D ** -0.5, 0.125, ((1, 4), (2, 4)))
    w_input = noise(streams_of[6], (2, D, KW), D ** -0.5, 0.125, ((1, 4), (2, 4)))
    w_gate = noise(streams_of[7], (2, D, KW), D ** -0.5, 0.125, ((1, 4), (2, 4)))
    w_out = noise(streams_of[8], (2, KW, D), KW ** -0.5, 0.125, ((1, 4), (2, 4)))
    bound_logit = draw_bound_logit(jax.random.fold_in(streams_of[12], 71), part)
    pace = jnp.clip(jnp.exp(math.log(2.0) - 1.2039728 * jax.random.uniform(streams_of[10], (2, KW), jnp.float32) ** levels(streams_of[10], (2, KW), ((1, 4),), -0.2, 0.2)), 0.6, 2.0)
    head_gain = jnp.clip(jnp.exp(jax.random.uniform(streams_of[11], (2, HEAD), jnp.float32, math.log(0.4), math.log(2.5))), 0.4, 2.5)
    return {"tokens": tokens, "state": state, "lengths": lengths, "norm_gain": norm_gain, "w_query": w_query, "w_forget": w_forget, "w_input": w_input, "w_gate": w_gate, "w_out": w_out, "bound_logit": bound_logit, "pace": pace, "head_gain": head_gain}


epsilon = 1e-06

def advance(prior, query, forget_in, value, gate, lower, pace_row, log_len, gain_row):
    count, width = query.shape
    size = prior.shape[-1]
    heads = width // size
    pre = forget_in - pace_row[None, :] * log_len[:, None]
    forget = lower[None, :] + (1.0 - lower[None, :]) * jax.nn.sigmoid(pre)
    key = (1.0 - lower[None, :]) * jax.nn.sigmoid(-pre)
    forget = forget.reshape(count, heads, size)
    key = key.reshape(count, heads, size)
    values = value.reshape(count, heads, size)
    updated = forget[..., None] * prior + key[..., None] * values[:, :, None, :]
    readout = jnp.einsum('bhk,bhkv->bhv', query.reshape(count, heads, size), updated, precision=lax.Precision.HIGHEST)
    normed = readout * lax.rsqrt(lax.optimization_barrier(jnp.mean(readout * readout, axis=-1, keepdims=True)) + epsilon)
    gates = gate.reshape(count, heads, size)
    normed = normed * gain_row[None, None, :] * jax.nn.silu(gates)
    return (updated, normed.reshape(count, width).astype(jnp.bfloat16))

def reference(tokens, state, lengths, norm_gain, w_query, w_forget, w_input, w_gate, w_out, bound_logit, pace, head_gain):
    current = tokens
    log_len = jnp.log(lengths.astype(jnp.float32) / LENGTH_MEAN)
    states = []
    result = None
    for block in range(2):
        wide = current.astype(jnp.float32)
        squares = lax.optimization_barrier(jnp.sum(wide * wide, axis=1))
        scale = lax.rsqrt(squares / D + epsilon)
        gained = (wide * norm_gain[block].astype(jnp.float32)[None, :]).astype(jnp.bfloat16)
        made = []
        for weight in (w_query[block], w_forget[block], w_input[block], w_gate[block]):
            made.append(scale[:, None] * jnp.dot(gained, weight, preferred_element_type=jnp.float32))
        lower = jax.nn.sigmoid(bound_logit[block])
        updated, normed = advance(state[block], made[0], made[1], made[2], made[3], lower, pace[block], log_len, head_gain[block])
        states.append(updated)
        branch = jnp.dot(normed, w_out[block], preferred_element_type=jnp.float32)
        if block == 0:
            current = (wide + branch).astype(jnp.bfloat16)
        else:
            result = wide + branch
    return (result, jnp.stack(states))
```

```python
import functools

import jax
import jax.numpy as jnp
from jax import lax
from jax.experimental import pallas as pl
from jax.experimental.pallas import tpu as pltpu
from jax.sharding import PartitionSpec as P

LENGTH_MEAN = 512
epsilon = 1e-06
GROUP = 8
LIMIT = 26 * 1024 * 1024
MESH_ID = pl.DeviceIdType.MESH
f32 = jnp.float32
bf16 = jnp.bfloat16


def chain(
    n_tp,
    n_dp,
    width,
    parts,
    tokens,
    state,
    lengths,
    gain,
    w_query,
    w_forget,
    w_input,
    w_gate,
    w_out,
    bound,
    pace,
    head_gain,
    mixed,
    sbuf,
    lengths_s,
    gain_s,
    bound_s,
    pace_s,
    hgain_s,
    forget_s,
    value_s,
    xall,
    wbuf,
    wobuf,
    pf,
    sq_s,
    psend,
    precv,
    relay,
    nall,
    po,
    osend,
    orecv,
    gate_s,
    qf_s,
    qk_s,
    ro_s,
    in_sem,
    t_sem,
    w_sem,
    s_sem,
    x_ss,
    x_rs,
    p_ss,
    p_rs,
    r_rs,
    n_ss,
    n_rs,
    o_ss,
    o_rs,
):
    t, d = lax.axis_index("tp"), lax.axis_index("dp")
    rt, feats = tokens.shape
    own, heads, size = state.shape[1], state.shape[2], state.shape[3]
    chans = heads * size
    hr, rh = own // parts, rt // parts
    rows_all = n_dp * hr
    per_part = hr // GROUP
    relayed = n_dp >= 4
    last = n_dp - 2
    at_end = jnp.logical_or(d == 0, d == n_dp - 1)
    merging = jnp.logical_or(d == 1, d == n_dp - 2)

    def tp_peer(k):
        return lax.rem(t + k, n_tp)

    def dp_peer(k):
        return lax.rem(d + k, n_dp)

    def start_all(copies):
        for c in copies:
            c.start()

    token_loads = [
        pltpu.make_async_copy(tokens.at[pl.ds(p * rh, rh)], xall.at[0, p, t], t_sem.at[p]) for p in range(parts)
    ]
    small = [
        pltpu.make_async_copy(src, dst, in_sem.at[i])
        for i, (src, dst) in enumerate(
            ((gain, gain_s), (lengths, lengths_s), (bound, bound_s), (pace, pace_s), (head_gain, hgain_s))
        )
    ]
    loads = []
    for b in range(2):
        per = []
        for i, w in enumerate((w_query, w_forget, w_input, w_gate)):
            per.append(pltpu.make_async_copy(w.at[b], wbuf.at[b, i], w_sem.at[b, i]))
        per.append(pltpu.make_async_copy(w_out.at[b], wobuf.at[b], w_sem.at[b, 4]))
        loads.append(per)

    def state_load(b, g):
        rows = pl.ds(g * GROUP, GROUP)
        return pltpu.make_async_copy(state.at[b, rows], sbuf.at[b, rows], s_sem.at[b, g])

    start_all(token_loads)
    start_all(small)
    start_all(loads[0])

    barrier = pltpu.get_barrier_semaphore()
    for k in range(1, n_tp):
        pl.semaphore_signal(barrier, inc=1, device_id={"tp": tp_peer(k)}, device_id_type=MESH_ID)
    for k in range(1, n_dp):
        pl.semaphore_signal(barrier, inc=1, device_id={"dp": dp_peer(k)}, device_id_type=MESH_ID)
    pl.semaphore_wait(barrier, n_tp + n_dp - 2)

    sends = []
    lane = lax.broadcasted_iota(jnp.int32, (hr, 128), 1)
    row_id = lax.broadcasted_iota(jnp.int32, (GROUP, size), 0)
    spread = jnp.where(
        lax.broadcasted_iota(jnp.int32, (GROUP, GROUP * size), 1) // size
        == lax.broadcasted_iota(jnp.int32, (GROUP, GROUP * size), 0),
        1.0,
        0.0,
    ).astype(bf16)
    spread = jnp.concatenate([spread] * 3, axis=0)

    def far_first(n):
        return [n // 2] + [k for k in range(1, n) if k != n // 2]

    def x_copy(b, p, k):
        return pltpu.make_async_remote_copy(
            src_ref=xall.at[b, p, t],
            dst_ref=xall.at[b, p, t],
            send_sem=x_ss.at[b, p, k - 1],
            recv_sem=x_rs.at[b, p, k - 1],
            device_id={"tp": tp_peer(k)},
            device_id_type=MESH_ID,
        )

    def share(b, p):
        for k in far_first(n_tp):
            c = x_copy(b, p, k)
            c.start()
            sends.append(c)

    def offset(i):
        if not relayed:
            return far_first(n_dp)[i]
        if i == last:
            middle = jnp.where(d == 1, n_dp - 2, jnp.where(d == n_dp - 2, 2, n_dp - 1))
        else:
            skip = jnp.where(d == 1, n_dp - 2, jnp.where(d == n_dp - 2, 2, n_dp - 1))
            middle = jnp.where(i + 1 < skip, i + 1, i + 2)
        return jnp.where(d == 0, n_dp - 1 - i, jnp.where(d == n_dp - 1, i + 1, middle))

    def partial_copy(b, p, k):
        dest = dp_peer(k)
        return pltpu.make_async_remote_copy(
            src_ref=psend.at[b, p, dest],
            dst_ref=precv.at[b, p, k - 1],
            send_sem=p_ss.at[b, p, k - 1],
            recv_sem=p_rs.at[b, p, k - 1],
            device_id={"dp": dest},
            device_id_type=MESH_ID,
        )

    def relay_copy(b, p, k):
        return pltpu.make_async_remote_copy(
            src_ref=psend.at[b, p, dp_peer(k)],
            dst_ref=relay.at[b, p],
            send_sem=p_ss.at[b, p, k - 1],
            recv_sem=r_rs.at[b, p],
            device_id={"dp": jnp.where(d == 0, 1, n_dp - 2)},
            device_id_type=MESH_ID,
        )

    def pack(sq):
        hi = sq.astype(bf16).astype(f32)
        return jnp.where(lane == 0, hi, jnp.where(lane == 1, sq - hi, 0.0)).astype(bf16)

    def send_step(b, p, i):
        k = offset(i)
        c = partial_copy(b, p, k)
        if relayed and i == 0:

            @pl.when(at_end)
            def _():
                relay_copy(b, p, k).start()

            @pl.when(jnp.logical_not(at_end))
            def _():
                c.start()

        else:
            if relayed and i == last:

                @pl.when(merging)
                def _():
                    relay_copy(b, p, k).wait_recv()
                    dest = dp_peer(k)
                    for j in range(4):
                        cols = slice(j * chans, (j + 1) * chans)
                        both = pf[p, dest, :, cols] + relay[b, p, :, cols].astype(f32)
                        psend[b, p, dest, :, cols] = both.astype(bf16)
                    far = jnp.sum(relay[b, p, :, 4 * chans :].astype(f32), axis=1, keepdims=True)
                    psend[b, p, dest, :, 4 * chans :] = pack(sq_s[p, dest] + far)

            c.start()
        sends.append(c)

    def project(b, p):
        if p == 0:
            for i in range(4):
                loads[b][i].wait()
        for k in range(1, n_tp):
            x_copy(b, p, k).wait_recv()
        x = xall[b, p].reshape(rows_all, feats).astype(f32)
        sq = jnp.sum(x * x, axis=1, keepdims=True)
        gained = (x * gain_s[b : b + 1, :].astype(f32)).astype(bf16)
        sq_s[p] = jnp.broadcast_to(sq, (rows_all, 128)).reshape(n_dp, hr, 128)
        for e in range(n_dp):
            psend[b, p, e, :, 4 * chans :] = pack(jnp.broadcast_to(sq[e * hr : (e + 1) * hr], (hr, 128)))
        for i in range(4):
            cols = slice(i * chans, (i + 1) * chans)
            part = jnp.dot(gained, wbuf[b, i], preferred_element_type=f32)
            pf[p, :, :, cols] = part.reshape(n_dp, hr, chans)
            psend[b, p, :, :, cols] = part.astype(bf16).reshape(n_dp, hr, chans)
        for i in range(last):
            send_step(b, p, i)

    def finish_sends(b, p):
        send_step(b, p, last)

    def gates(b, p):
        if b == 0 and p == 0:
            for c in small[1:]:
                c.wait()
        for k in range(1, n_dp):
            c = partial_copy(b, p, k)
            if relayed and k == 1:
                pl.when(d != 0)(c.wait_recv)
            elif relayed and k == n_dp - 1:
                pl.when(d != n_dp - 1)(c.wait_recv)
            else:
                c.wait_recv()

        squares = sq_s[p, d, :, :1]
        for k in range(n_dp - 1):
            squares = squares + jnp.sum(precv[b, p, k, :, 4 * chans :].astype(f32), axis=1, keepdims=True)
        scale = lax.rsqrt(squares / width + epsilon)

        def total(i):
            cols = slice(i * chans, (i + 1) * chans)
            acc = pf[p, d, :, cols]
            for k in range(n_dp - 1):
                acc = acc + precv[b, p, k, :, cols].astype(f32)
            return scale * acc

        rows = slice(p * hr, (p + 1) * hr)
        log_row = jnp.log(lengths_s[...].astype(f32) / LENGTH_MEAN)
        pick = lax.broadcasted_iota(jnp.int32, (hr, own), 1) == lax.broadcasted_iota(jnp.int32, (hr, own), 0) + p * hr
        log_len = jnp.sum(jnp.where(pick, log_row, 0.0), axis=1, keepdims=True)
        lower = jax.nn.sigmoid(bound_s[b : b + 1, :])
        pre = total(1) - pace_s[b : b + 1, :] * log_len
        forget = lower + (1.0 - lower) * jax.nn.sigmoid(pre)
        key = (1.0 - lower) * jax.nn.sigmoid(-pre)
        forget_s[b, rows] = forget
        query = total(0)
        qf_s[...] = query * forget
        qk_s[...] = query * key
        value_s[b, rows] = total(2)
        gate = total(3)
        gate_s[...] = gate * jax.nn.sigmoid(gate)

        for g in range(per_part):
            state_load(b, p * per_part + g).wait()

        def read(g, carry):
            at = pl.ds(pl.multiple_of(g * GROUP, GROUP), GROUP)
            seqs = pl.ds(pl.multiple_of(p * hr + g * GROUP, GROUP), GROUP)
            for h in range(heads):
                cols = slice(h * size, (h + 1) * size)
                q8 = qf_s[at, cols]
                diag = jnp.concatenate(
                    [jnp.where(row_id == j, q8, 0.0) for j in range(GROUP)], axis=1
                ).astype(bf16)
                s8 = sbuf[b, seqs, h].reshape(GROUP * size, size).astype(bf16)
                ro_s[at, cols] = jnp.dot(diag, s8, preferred_element_type=f32)
            return carry

        lax.fori_loop(0, per_part, read, 0)
        for h in range(heads):
            cols = slice(h * size, (h + 1) * size)
            dots = jnp.sum(qk_s[:, cols], axis=1, keepdims=True)
            readout = ro_s[:, cols] + dots * value_s[b, rows, cols]
            mean = jnp.mean(readout * readout, axis=1, keepdims=True)
            normed = readout * lax.rsqrt(mean + epsilon) * hgain_s[b : b + 1, :] * gate_s[:, cols]
            nall[b, p, d, :, cols] = normed.astype(bf16)
        for k in far_first(n_dp):
            c = normed_copy(b, p, k)
            c.start()
            sends.append(c)

    def normed_copy(b, p, k):
        return pltpu.make_async_remote_copy(
            src_ref=nall.at[b, p, d],
            dst_ref=nall.at[b, p, d],
            send_sem=n_ss.at[b, p, k - 1],
            recv_sem=n_rs.at[b, p, k - 1],
            device_id={"dp": dp_peer(k)},
            device_id_type=MESH_ID,
        )

    def out_copy(b, p, k):
        dest = tp_peer(k)
        return pltpu.make_async_remote_copy(
            src_ref=osend.at[b, p, dest],
            dst_ref=orecv.at[b, p, k - 1],
            send_sem=o_ss.at[b, p, k - 1],
            recv_sem=o_rs.at[b, p, k - 1],
            device_id={"tp": dest},
            device_id_type=MESH_ID,
        )

    def out_project(b, p):
        if p == 0:
            loads[b][4].wait()
        for k in range(1, n_dp):
            normed_copy(b, p, k).wait_recv()
        rows = nall[b, p].reshape(rows_all, chans)
        part = jnp.dot(rows, wobuf[b], preferred_element_type=f32)
        po[p] = part.reshape(n_tp, rh, feats)
        osend[b, p] = part.astype(bf16).reshape(n_tp, rh, feats)
        for k in far_first(n_tp):
            c = out_copy(b, p, k)
            c.start()
            sends.append(c)

    def residual(b, p):
        for k in range(1, n_tp):
            out_copy(b, p, k).wait_recv()
        branch = po[p, t]
        for k in range(n_tp - 1):
            branch = branch + orecv[b, p, k].astype(f32)
        result = xall[b, p, t].astype(f32) + branch
        if b == 0:
            xall[1, p, t] = result.astype(bf16)
            share(1, p)
        else:
            mixed[p * rh : (p + 1) * rh, :] = result

    def advance(b, p):
        def step(g, carry):
            base = pl.multiple_of(p * hr + g * GROUP, GROUP)
            rows = pl.ds(base, GROUP)
            f = forget_s[b, rows, :]
            top = f.astype(bf16)
            rest = f - top.astype(f32)
            mid = rest.astype(bf16)
            low = (rest - mid.astype(f32)).astype(bf16)
            pieces = jnp.concatenate([top, mid, low], axis=0)
            for h in range(heads):
                cols = slice(h * size, (h + 1) * size)
                v = value_s[b, rows, cols]
                for j in range(0, GROUP, 2):
                    wide = lax.dot_general(
                        pieces[:, cols],
                        spread[:, j * size : (j + 2) * size],
                        (((0,), (0,)), ((), ())),
                        preferred_element_type=f32,
                    )
                    for i in range(2):
                        row = v[j + i : j + i + 1, :]
                        keep = wide[:, i * size : (i + 1) * size]
                        sbuf[b, base + j + i, h] = row + keep * (sbuf[b, base + j + i, h] - row)
            return carry

        lax.fori_loop(0, per_part, step, 0)

    if relayed:
        for k, end in ((1, 0), (n_dp - 1, n_dp - 1)):

            @pl.when(d == end)
            def _():
                for b in range(2):
                    for p in range(parts):
                        precv[b, p, k - 1] = jnp.zeros(precv.shape[3:], bf16)

    for p in range(parts):
        token_loads[p].wait()
        share(0, p)
    for g in range(own // GROUP):
        state_load(0, g).start()
    start_all(loads[1])
    for g in range(own // GROUP):
        state_load(1, g).start()
    small[0].wait()

    if parts == 1:
        order = []
        for b in range(2):
            order += [(f, b, 0) for f in (project, finish_sends, gates, advance, out_project, residual)]
    else:
        order = [
            (project, 0, 0),
            (finish_sends, 0, 0),
            (project, 0, 1),
            (gates, 0, 0),
            (finish_sends, 0, 1),
            (advance, 0, 0),
            (out_project, 0, 0),
            (gates, 0, 1),
            (residual, 0, 0),
            (project, 1, 0),
            (advance, 0, 1),
            (out_project, 0, 1),
            (finish_sends, 1, 0),
            (residual, 0, 1),
            (project, 1, 1),
            (gates, 1, 0),
            (finish_sends, 1, 1),
            (advance, 1, 0),
            (out_project, 1, 0),
            (gates, 1, 1),
            (residual, 1, 0),
            (advance, 1, 1),
            (out_project, 1, 1),
            (residual, 1, 1),
        ]
    for f, b, p in order:
        f(b, p)

    for c in sends:
        c.wait_send()


def store(mixed, new_state, mixed_out, state_out, sems):
    blocks, own = new_state.shape[:2]
    copies = [pltpu.make_async_copy(mixed, mixed_out, sems.at[blocks, 0])]
    for b in range(blocks):
        for g in range(own // GROUP):
            rows = pl.ds(g * GROUP, GROUP)
            copies.append(pltpu.make_async_copy(new_state.at[b, rows], state_out.at[b, rows], sems.at[b, g]))
    for c in copies:
        c.start()
    for c in copies:
        c.wait()


def shards(n_tp, n_dp, tokens, state, lengths, gain, w_query, w_forget, w_input, w_gate, w_out, bound, pace, head_gain):
    rt, feats = tokens.shape
    own, heads, size = state.shape[1:4]
    chans = heads * size
    parts = 2 if own == rt and own % (4 * GROUP) == 0 else 1
    hr, rh = own // parts, rt // parts
    msg = 4 * chans + 128
    vmem = pl.BlockSpec(memory_space=pltpu.VMEM)
    hbm = pl.BlockSpec(memory_space=pl.ANY)
    dma = pltpu.SemaphoreType.DMA
    mixed, new_state = pl.pallas_call(
        functools.partial(chain, n_tp, n_dp, feats * n_dp, parts),
        name="chain",
        out_shape=(pltpu.VMEM((rt, feats), f32), pltpu.VMEM(state.shape, f32)),
        in_specs=[hbm] * 12,
        out_specs=(vmem, vmem),
        scratch_shapes=[
            pltpu.VMEM((1, own), jnp.int32),
            pltpu.VMEM(gain.shape, bf16),
            pltpu.VMEM(bound.shape, f32),
            pltpu.VMEM(pace.shape, f32),
            pltpu.VMEM(head_gain.shape, f32),
            pltpu.VMEM((2, own, chans), f32),
            pltpu.VMEM((2, own, chans), f32),
            pltpu.VMEM((2, parts, n_tp, rh, feats), bf16),
            pltpu.VMEM((2, 4, feats, chans), bf16),
            pltpu.VMEM((2, chans, feats), bf16),
            pltpu.VMEM((parts, n_dp, hr, 4 * chans), f32),
            pltpu.VMEM((parts, n_dp, hr, 128), f32),
            pltpu.VMEM((2, parts, n_dp, hr, msg), bf16),
            pltpu.VMEM((2, parts, n_dp - 1, hr, msg), bf16),
            pltpu.VMEM((2, parts, hr, msg), bf16),
            pltpu.VMEM((2, parts, n_dp, hr, chans), bf16),
            pltpu.VMEM((parts, n_tp, rh, feats), f32),
            pltpu.VMEM((2, parts, n_tp, rh, feats), bf16),
            pltpu.VMEM((2, parts, n_tp - 1, rh, feats), bf16),
            pltpu.VMEM((hr, chans), f32),
            pltpu.VMEM((hr, chans), f32),
            pltpu.VMEM((hr, chans), f32),
            pltpu.VMEM((hr, chans), f32),
            dma((5,)),
            dma((parts,)),
            dma((2, 5)),
            dma((2, own // GROUP)),
            dma((2, parts, n_tp - 1)),
            dma((2, parts, n_tp - 1)),
            dma((2, parts, n_dp - 1)),
            dma((2, parts, n_dp - 1)),
            dma((2, parts)),
            dma((2, parts, n_dp - 1)),
            dma((2, parts, n_dp - 1)),
            dma((2, parts, n_tp - 1)),
            dma((2, parts, n_tp - 1)),
        ],
        compiler_params=pltpu.CompilerParams(
            collective_id=0, has_side_effects=True, vmem_limit_bytes=LIMIT
        ),
    )(tokens, state, lengths[None, :], gain, w_query, w_forget, w_input, w_gate, w_out, bound, pace, head_gain)

    return pl.pallas_call(
        store,
        name="store",
        out_shape=(jax.ShapeDtypeStruct((rt, feats), f32), jax.ShapeDtypeStruct(state.shape, f32)),
        in_specs=[vmem, vmem],
        out_specs=(hbm, hbm),
        scratch_shapes=[dma((3, own // GROUP))],
        compiler_params=pltpu.CompilerParams(vmem_limit_bytes=LIMIT),
    )(pltpu.with_memory_space_constraint(mixed, pltpu.VMEM), pltpu.with_memory_space_constraint(new_state, pltpu.VMEM))


def solution(mesh):
    in_specs = (
        P(("grp", "tp"), "dp"),
        P(None, ("grp", "dp"), "tp", None, None),
        P(("grp", "dp")),
        P(None, "dp"),
        P(None, "dp", "tp"),
        P(None, "dp", "tp"),
        P(None, "dp", "tp"),
        P(None, "dp", "tp"),
        P(None, "tp", "dp"),
        P(None, "tp"),
        P(None, "tp"),
        P(),
    )
    out_specs = (P(("grp", "tp"), "dp"), P(None, ("grp", "dp"), "tp", None, None))
    body = functools.partial(shards, mesh.shape["tp"], mesh.shape["dp"])
    return jax.shard_map(body, mesh=mesh, in_specs=in_specs, out_specs=out_specs, check_vma=False)
```

```python
import functools

import jax
import jax.numpy as jnp
from jax import lax
from jax.experimental import pallas as pl
from jax.experimental.pallas import tpu as pltpu
from jax.sharding import PartitionSpec as P

LENGTH_MEAN = 512
epsilon = 1e-06
GROUP = 8
PARTS = 4
RELAYS = 2
LIMIT = 26 * 1024 * 1024
MESH_ID = pl.DeviceIdType.MESH
f32 = jnp.float32
bf16 = jnp.bfloat16


ORDER = (
    "P0", "P1", "E0", "E1", "M0", "N0", "M1", "N1", "G0", "A0", "P2", "G1", "A1", "P3", "E2", "E3", "O0",
    "M2", "N2", "M3", "Z0", "N3", "G2", "A2", "O1", "Y0", "P4", "Z1", "G3", "A3", "V3", "O2", "E4", "Y1",
    "P5", "M4", "E5", "Z2", "O3", "M5", "Z3", "Y2", "N4", "N5", "P6", "Y3", "P7", "E6", "M6", "E7", "N6",
    "G5", "M7", "V2", "N7", "V1", "G4", "A4", "V0", "A5", "G6", "A6", "G7", "A7", "O4", "O5", "V4", "O6",
    "O7", "V6", "Y4", "V5", "V7", "Y6", "Y5", "Y7",
)


def chain(
    n_tp,
    n_dp,
    width,
    parts,
    tokens,
    state,
    lengths,
    gain,
    w_query,
    w_forget,
    w_input,
    w_gate,
    w_out,
    bound,
    pace,
    head_gain,
    mixed,
    sbuf,
    lengths_s,
    gain_s,
    bound_s,
    pace_s,
    hgain_s,
    forget_s,
    value_s,
    xall,
    wbuf,
    wobuf,
    pf,
    sqx,
    psend,
    precv,
    relay,
    nall,
    po,
    osend,
    orecv,
    pair,
    zsend,
    zrecv,
    gate_s,
    qf_s,
    qk_s,
    ro_s,
    in_sem,
    t_sem,
    w_sem,
    s_sem,
    x_ss,
    x_rs,
    p_ss,
    p_rs,
    r_rs,
    q_ss,
    q_rs,
    n_ss,
    n_rs,
    o_ss,
    o_rs,
    d_ss,
    d_rs,
    z_ss,
    z_rs,
):
    t, d = lax.axis_index("tp"), lax.axis_index("dp")
    rt, feats = tokens.shape
    own, heads, size = state.shape[1], state.shape[2], state.shape[3]
    chans = heads * size
    hr, rh = own // parts, rt // parts
    rows_all = n_dp * hr
    per_part = hr // GROUP
    relayed = n_dp >= 4
    hops = min(RELAYS, n_dp - 2)
    core, chip, chips = lax.rem(t, 2), lax.div(t, 2), n_tp // 2
    at_end = jnp.logical_or(d == 0, d == n_dp - 1)
    merging = jnp.logical_or(d == 1, d == n_dp - 2)

    def tp_peer(k):
        return lax.rem(t + k, n_tp)

    def dp_peer(k):
        return lax.rem(d + k, n_dp)

    def start_all(copies):
        for c in copies:
            c.start()

    token_loads = [
        pltpu.make_async_copy(tokens.at[pl.ds(p * rh, rh)], xall.at[0, p, t], t_sem.at[p]) for p in range(parts)
    ]
    small = [
        pltpu.make_async_copy(src, dst, in_sem.at[i])
        for i, (src, dst) in enumerate(
            ((gain, gain_s), (lengths, lengths_s), (bound, bound_s), (pace, pace_s), (head_gain, hgain_s))
        )
    ]
    loads = []
    for b in range(2):
        per = []
        for i, w in enumerate((w_query, w_forget, w_input, w_gate)):
            per.append(pltpu.make_async_copy(w.at[b], wbuf.at[b, i], w_sem.at[b, i]))
        per.append(pltpu.make_async_copy(w_out.at[b], wobuf.at[b], w_sem.at[b, 4]))
        loads.append(per)

    def state_load(b, g):
        rows = pl.ds(g * GROUP, GROUP)
        return pltpu.make_async_copy(state.at[b, rows], sbuf.at[b, rows], s_sem.at[b, g])

    start_all(token_loads)
    start_all(small)
    start_all(loads[0])

    barrier = pltpu.get_barrier_semaphore()
    for k in range(1, n_tp):
        pl.semaphore_signal(barrier, inc=1, device_id={"tp": tp_peer(k)}, device_id_type=MESH_ID)
    for k in range(1, n_dp):
        pl.semaphore_signal(barrier, inc=1, device_id={"dp": dp_peer(k)}, device_id_type=MESH_ID)
    pl.semaphore_wait(barrier, n_tp + n_dp - 2)

    sends = []
    row_id = lax.broadcasted_iota(jnp.int32, (GROUP, size), 0)
    spread = jnp.where(
        lax.broadcasted_iota(jnp.int32, (GROUP, GROUP * size), 1) // size
        == lax.broadcasted_iota(jnp.int32, (GROUP, GROUP * size), 0),
        1.0,
        0.0,
    ).astype(bf16)
    spread = jnp.concatenate([spread] * 3, axis=0)

    def far_first(n):
        return [n // 2] + [k for k in range(1, n) if k != n // 2]

    def x_copy(b, p, k):
        return pltpu.make_async_remote_copy(
            src_ref=xall.at[b, p, t],
            dst_ref=xall.at[b, p, t],
            send_sem=x_ss.at[b, p, k - 1],
            recv_sem=x_rs.at[b, p, k - 1],
            device_id={"tp": tp_peer(k)},
            device_id_type=MESH_ID,
        )

    def share(b, p):
        for k in far_first(n_tp):
            c = x_copy(b, p, k)
            c.start()
            sends.append(c)

    def partial_copy(b, p, k):
        dest = dp_peer(k)
        return pltpu.make_async_remote_copy(
            src_ref=psend.at[b, p, dest],
            dst_ref=precv.at[b, p, k - 1],
            send_sem=p_ss.at[b, p, k - 1],
            recv_sem=p_rs.at[b, p, k - 1],
            device_id={"dp": dest},
            device_id_type=MESH_ID,
        )

    def relay_copy(b, p, k, i):
        return pltpu.make_async_remote_copy(
            src_ref=psend.at[b, p, dp_peer(k)],
            dst_ref=relay.at[b, p, i],
            send_sem=p_ss.at[b, p, k - 1],
            recv_sem=r_rs.at[b, p, i],
            device_id={"dp": jnp.where(d == 0, 1, n_dp - 2)},
            device_id_type=MESH_ID,
        )

    def square_copy(b, p, k):
        return pltpu.make_async_remote_copy(
            src_ref=sqx.at[b, p, d],
            dst_ref=sqx.at[b, p, d],
            send_sem=q_ss.at[b, p, k - 1],
            recv_sem=q_rs.at[b, p, k - 1],
            device_id={"dp": dp_peer(k)},
            device_id_type=MESH_ID,
        )

    def far_along(i):
        middle = far_first(n_dp)[i]
        return jnp.where(d == 0, n_dp - 1 - i, jnp.where(d == n_dp - 1, i + 1, middle))

    def send_partials(b, p):
        for k in range(1, n_dp):
            sends.append(partial_copy(b, p, k))
        if not relayed:
            for k in far_first(n_dp):
                partial_copy(b, p, k).start()
            return

        @pl.when(at_end)
        def _():
            for i in range(n_dp - 2):
                k = jnp.where(d == 0, n_dp - 1 - i, i + 1)
                c = relay_copy(b, p, k, i) if i < hops else partial_copy(b, p, k)
                c.start()

        @pl.when(merging)
        def _():
            for i in range(n_dp - 1 - hops):
                k = jnp.where(d == 1, i, n_dp - i) if i else jnp.where(d == 1, n_dp - 1, 1)
                partial_copy(b, p, k).start()

        if n_dp > 4:

            @pl.when(jnp.logical_not(jnp.logical_or(at_end, merging)))
            def _():
                for k in far_first(n_dp):
                    partial_copy(b, p, k).start()

    def finish_ends(b, p):
        if relayed:
            pl.when(at_end)(partial_copy(b, p, jnp.where(d == 0, 1, n_dp - 1)).start)

    def merge(b, p, i):
        @pl.when(merging)
        def _():
            dest = jnp.where(d == 1, n_dp - 1 - i, i)
            k = lax.rem(dest - d + n_dp, n_dp)
            relay_copy(b, p, k, i).wait_recv()
            for j in range(4):
                cols = slice(j * chans, (j + 1) * chans)
                both = pf[p, dest, :, cols] + relay[b, p, i, :, cols].astype(f32)
                psend[b, p, dest, :, cols] = both.astype(bf16)
            partial_copy(b, p, k).start()

    def merge_far(b, p):
        if relayed:
            merge(b, p, 0)

    def merge_near(b, p):
        if relayed:
            for i in range(1, hops):
                merge(b, p, i)

    def bypassed(k):
        source = lax.rem(d - k + n_dp, n_dp)
        low = jnp.logical_and(source == 0, d >= n_dp - hops)
        return jnp.logical_or(low, jnp.logical_and(source == n_dp - 1, d < hops))

    def project(b, p):
        if p == 0:
            for i in range(4):
                loads[b][i].wait()
        if b == 0:
            for k in range(1, n_tp):
                x_copy(b, p, k).wait_recv()
        x = xall[b, p].reshape(rows_all, feats).astype(f32)
        sq = jnp.sum(x * x, axis=1, keepdims=True)
        gained = (x * gain_s[b : b + 1, :].astype(f32)).astype(bf16)
        square = lax.broadcasted_iota(jnp.int32, (rows_all, rows_all), 0) == lax.broadcasted_iota(
            jnp.int32, (rows_all, rows_all), 1
        )
        sqx[b, p, d] = jnp.sum(jnp.where(square, sq, 0.0), axis=0, keepdims=True)
        for i in range(n_dp - 1):
            c = square_copy(b, p, far_along(i))
            c.start()
            sends.append(c)
        for i in range(4):
            cols = slice(i * chans, (i + 1) * chans)
            part = jnp.dot(gained, wbuf[b, i], preferred_element_type=f32)
            pf[p, :, :, cols] = part.reshape(n_dp, hr, chans)
            psend[b, p, :, :, cols] = part.astype(bf16).reshape(n_dp, hr, chans)
        send_partials(b, p)

    def gates(b, p):
        if b == 0 and p == 0:
            for c in small[1:]:
                c.wait()
        for k in range(1, n_dp):
            c = partial_copy(b, p, k)
            if relayed:
                pl.when(jnp.logical_not(bypassed(k)))(c.wait_recv)
            else:
                c.wait_recv()

        for k in range(1, n_dp):
            square_copy(b, p, k).wait_recv()
        row = sqx[b, p, 0]
        for e in range(1, n_dp):
            row = row + sqx[b, p, e]
        mine = (
            lax.broadcasted_iota(jnp.int32, (hr, rows_all), 1)
            == lax.broadcasted_iota(jnp.int32, (hr, rows_all), 0) + d * hr
        )
        squares = jnp.sum(jnp.where(mine, row, 0.0), axis=1, keepdims=True)
        scale = lax.rsqrt(squares / width + epsilon)

        def total(i):
            cols = slice(i * chans, (i + 1) * chans)
            acc = pf[p, d, :, cols]
            for k in range(n_dp - 1):
                acc = acc + precv[b, p, k, :, cols].astype(f32)
            return scale * acc

        rows = slice(p * hr, (p + 1) * hr)
        log_row = jnp.log(lengths_s[...].astype(f32) / LENGTH_MEAN)
        pick = lax.broadcasted_iota(jnp.int32, (hr, own), 1) == lax.broadcasted_iota(jnp.int32, (hr, own), 0) + p * hr
        log_len = jnp.sum(jnp.where(pick, log_row, 0.0), axis=1, keepdims=True)
        lower = jax.nn.sigmoid(bound_s[b : b + 1, :])
        pre = total(1) - pace_s[b : b + 1, :] * log_len
        forget = lower + (1.0 - lower) * jax.nn.sigmoid(pre)
        key = (1.0 - lower) * jax.nn.sigmoid(-pre)
        forget_s[b, rows] = forget
        query = total(0)
        qf_s[...] = query * forget
        qk_s[...] = query * key
        value_s[b, rows] = total(2)
        gate = total(3)
        gate_s[...] = gate * jax.nn.sigmoid(gate)

        for g in range(per_part):
            state_load(b, p * per_part + g).wait()

        def read(g, carry):
            at = pl.ds(pl.multiple_of(g * GROUP, GROUP), GROUP)
            seqs = pl.ds(pl.multiple_of(p * hr + g * GROUP, GROUP), GROUP)
            for h in range(heads):
                cols = slice(h * size, (h + 1) * size)
                q8 = qf_s[at, cols]
                diag = jnp.concatenate(
                    [jnp.where(row_id == j, q8, 0.0) for j in range(GROUP)], axis=1
                ).astype(bf16)
                s8 = sbuf[b, seqs, h].reshape(GROUP * size, size).astype(bf16)
                ro_s[at, cols] = jnp.dot(diag, s8, preferred_element_type=f32)
            return carry

        lax.fori_loop(0, per_part, read, 0)
        for h in range(heads):
            cols = slice(h * size, (h + 1) * size)
            dots = jnp.sum(qk_s[:, cols], axis=1, keepdims=True)
            readout = ro_s[:, cols] + dots * value_s[b, rows, cols]
            mean = jnp.mean(readout * readout, axis=1, keepdims=True)
            normed = readout * lax.rsqrt(mean + epsilon) * hgain_s[b : b + 1, :] * gate_s[:, cols]
            nall[b, p, d, :, cols] = normed.astype(bf16)
    def share_normed(b, p):
        for i in range(n_dp - 1):
            c = normed_copy(b, p, far_along(i))
            c.start()
            sends.append(c)

    def normed_copy(b, p, k):
        return pltpu.make_async_remote_copy(
            src_ref=nall.at[b, p, d],
            dst_ref=nall.at[b, p, d],
            send_sem=n_ss.at[b, p, k - 1],
            recv_sem=n_rs.at[b, p, k - 1],
            device_id={"dp": dp_peer(k)},
            device_id_type=MESH_ID,
        )

    def out_copy(b, p, k):
        dest = tp_peer(k)
        return pltpu.make_async_remote_copy(
            src_ref=osend.at[b, p, dest],
            dst_ref=orecv.at[p, k - 1],
            send_sem=o_ss.at[p, k - 1],
            recv_sem=o_rs.at[p, k - 1],
            device_id={"tp": dest},
            device_id_type=MESH_ID,
        )

    def out_project(b, p):
        if p == 0:
            loads[b][4].wait()
        for k in range(1, n_dp):
            normed_copy(b, p, k).wait_recv()
        rows = nall[b, p].reshape(rows_all, chans)
        part = jnp.dot(rows, wobuf[b], preferred_element_type=f32)
        po[p] = part.reshape(n_tp, rh, feats)
        osend[b, p] = part.astype(bf16).reshape(n_tp, rh, feats)
        if b == 0:
            c = pair_copy(p)
            c.start()
            sends.append(c)
            return
        for k in far_first(n_tp):
            c = out_copy(b, p, k)
            c.start()
            sends.append(c)

    def pair_copy(p):
        return pltpu.make_async_remote_copy(
            src_ref=osend.at[0, p],
            dst_ref=pair.at[p],
            send_sem=d_ss.at[p],
            recv_sem=d_rs.at[p],
            device_id={"tp": t + 1 - 2 * core},
            device_id_type=MESH_ID,
        )

    def cross_copy(p, i):
        return pltpu.make_async_remote_copy(
            src_ref=zsend.at[p],
            dst_ref=zrecv.at[p, i // 2, core],
            send_sem=z_ss.at[p, i],
            recv_sem=z_rs.at[p, i // 2, core],
            device_id={"tp": lax.rem(2 * chip + i + 2, n_tp)},
            device_id_type=MESH_ID,
        )

    def cross_wait(p, i, c):
        arrived = pltpu.make_async_remote_copy(
            src_ref=zsend.at[p],
            dst_ref=zrecv.at[p, i, c],
            send_sem=z_ss.at[p, i],
            recv_sem=z_rs.at[p, i, c],
            device_id={"tp": lax.rem(t + 1, n_tp)},
            device_id_type=MESH_ID,
        )
        arrived.wait_recv()

    def cross(b, p):
        if b == 1:
            return
        pair_copy(p).wait_recv()
        po[p] = po[p] + pair[p].astype(f32)
        zsend[p] = po[p, pl.ds(core * chips, chips)].astype(bf16)
        for i in range(n_tp - 2):
            c = cross_copy(p, i)
            c.start()
            sends.append(c)

    def residual(b, p):
        if b == 0:
            for c in range(2):
                half = slice(c * chips, (c + 1) * chips)
                branch = po[p, half]
                for i in range(chips - 1):
                    cross_wait(p, i, c)
                    branch = branch + zrecv[p, i, c].astype(f32)
                xall[1, p, half] = (xall[0, p, half].astype(f32) + branch).astype(bf16)
            return
        for k in range(1, n_tp):
            out_copy(b, p, k).wait_recv()
        branch = po[p, t]
        for k in range(n_tp - 1):
            branch = branch + orecv[p, k].astype(f32)
        mixed[p * rh : (p + 1) * rh, :] = xall[b, p, t].astype(f32) + branch

    def advance(b, p):
        def step(g, carry):
            base = pl.multiple_of(p * hr + g * GROUP, GROUP)
            rows = pl.ds(base, GROUP)
            f = forget_s[b, rows, :]
            top = f.astype(bf16)
            rest = f - top.astype(f32)
            mid = rest.astype(bf16)
            low = (rest - mid.astype(f32)).astype(bf16)
            pieces = jnp.concatenate([top, mid, low], axis=0)
            for h in range(heads):
                cols = slice(h * size, (h + 1) * size)
                v = value_s[b, rows, cols]
                for j in range(0, GROUP, 2):
                    wide = lax.dot_general(
                        pieces[:, cols],
                        spread[:, j * size : (j + 2) * size],
                        (((0,), (0,)), ((), ())),
                        preferred_element_type=f32,
                    )
                    for i in range(2):
                        row = v[j + i : j + i + 1, :]
                        keep = wide[:, i * size : (i + 1) * size]
                        sbuf[b, base + j + i, h] = row + keep * (sbuf[b, base + j + i, h] - row)
            return carry

        lax.fori_loop(0, per_part, step, 0)

    if relayed:
        for k in range(1, n_dp):

            @pl.when(bypassed(k))
            def _():
                for b in range(2):
                    for p in range(parts):
                        precv[b, p, k - 1] = jnp.zeros(precv.shape[3:], bf16)

    for p in range(parts):
        token_loads[p].wait()
        share(0, p)
    for g in range(own // GROUP):
        state_load(0, g).start()
    start_all(loads[1])
    for g in range(own // GROUP):
        state_load(1, g).start()
    small[0].wait()

    if parts == 1:
        order = [(f, k) for k in range(2) for f in "PEMNGAVOZY"]
    else:
        order = [(step[0], int(step[1:])) for step in ORDER]
    stages = dict(
        P=project,
        E=finish_ends,
        M=merge_far,
        N=merge_near,
        G=gates,
        A=share_normed,
        O=out_project,
        Z=cross,
        Y=residual,
        V=advance,
    )
    for name, k in order:
        f, b, p = stages[name], k // parts, k % parts
        f(b, p)

    for c in sends:
        c.wait_send()


def store(mixed, new_state, mixed_out, state_out, sems):
    blocks, own = new_state.shape[:2]
    copies = [pltpu.make_async_copy(mixed, mixed_out, sems.at[blocks, 0])]
    for b in range(blocks):
        for g in range(own // GROUP):
            rows = pl.ds(g * GROUP, GROUP)
            copies.append(pltpu.make_async_copy(new_state.at[b, rows], state_out.at[b, rows], sems.at[b, g]))
    for c in copies:
        c.start()
    for c in copies:
        c.wait()


def shards(n_tp, n_dp, tokens, state, lengths, gain, w_query, w_forget, w_input, w_gate, w_out, bound, pace, head_gain):
    rt, feats = tokens.shape
    own, heads, size = state.shape[1:4]
    chans = heads * size
    parts = PARTS if own == rt and own % (2 * GROUP * PARTS) == 0 else 1
    hr, rh = own // parts, rt // parts
    msg = 4 * chans
    vmem = pl.BlockSpec(memory_space=pltpu.VMEM)
    hbm = pl.BlockSpec(memory_space=pl.ANY)
    dma = pltpu.SemaphoreType.DMA
    mixed, new_state = pl.pallas_call(
        functools.partial(chain, n_tp, n_dp, feats * n_dp, parts),
        name="chain",
        out_shape=(pltpu.VMEM((rt, feats), f32), pltpu.VMEM(state.shape, f32)),
        in_specs=[hbm] * 12,
        out_specs=(vmem, vmem),
        scratch_shapes=[
            pltpu.VMEM((1, own), jnp.int32),
            pltpu.VMEM(gain.shape, bf16),
            pltpu.VMEM(bound.shape, f32),
            pltpu.VMEM(pace.shape, f32),
            pltpu.VMEM(head_gain.shape, f32),
            pltpu.VMEM((2, own, chans), f32),
            pltpu.VMEM((2, own, chans), f32),
            pltpu.VMEM((2, parts, n_tp, rh, feats), bf16),
            pltpu.VMEM((2, 4, feats, chans), bf16),
            pltpu.VMEM((2, chans, feats), bf16),
            pltpu.VMEM((parts, n_dp, hr, 4 * chans), f32),
            pltpu.VMEM((2, parts, n_dp, 1, n_dp * hr), f32),
            pltpu.VMEM((2, parts, n_dp, hr, msg), bf16),
            pltpu.VMEM((2, parts, n_dp - 1, hr, msg), bf16),
            pltpu.VMEM((2, parts, max(n_dp - 2, 1), hr, msg), bf16),
            pltpu.VMEM((2, parts, n_dp, hr, chans), bf16),
            pltpu.VMEM((parts, n_tp, rh, feats), f32),
            pltpu.VMEM((2, parts, n_tp, rh, feats), bf16),
            pltpu.VMEM((parts, n_tp - 1, rh, feats), bf16),
            pltpu.VMEM((parts, n_tp, rh, feats), bf16),
            pltpu.VMEM((parts, n_tp // 2, rh, feats), bf16),
            pltpu.VMEM((parts, n_tp // 2 - 1, 2, n_tp // 2, rh, feats), bf16),
            pltpu.VMEM((hr, chans), f32),
            pltpu.VMEM((hr, chans), f32),
            pltpu.VMEM((hr, chans), f32),
            pltpu.VMEM((hr, chans), f32),
            dma((5,)),
            dma((parts,)),
            dma((2, 5)),
            dma((2, own // GROUP)),
            dma((2, parts, n_tp - 1)),
            dma((2, parts, n_tp - 1)),
            dma((2, parts, n_dp - 1)),
            dma((2, parts, n_dp - 1)),
            dma((2, parts, max(n_dp - 2, 1))),
            dma((2, parts, n_dp - 1)),
            dma((2, parts, n_dp - 1)),
            dma((2, parts, n_dp - 1)),
            dma((2, parts, n_dp - 1)),
            dma((parts, n_tp - 1)),
            dma((parts, n_tp - 1)),
            dma((parts,)),
            dma((parts,)),
            dma((parts, n_tp - 2)),
            dma((parts, n_tp // 2 - 1, 2)),
        ],
        compiler_params=pltpu.CompilerParams(
            collective_id=0, has_side_effects=True, vmem_limit_bytes=LIMIT
        ),
    )(tokens, state, lengths[None, :], gain, w_query, w_forget, w_input, w_gate, w_out, bound, pace, head_gain)

    return pl.pallas_call(
        store,
        name="store",
        out_shape=(jax.ShapeDtypeStruct((rt, feats), f32), jax.ShapeDtypeStruct(state.shape, f32)),
        in_specs=[vmem, vmem],
        out_specs=(hbm, hbm),
        scratch_shapes=[dma((3, own // GROUP))],
        compiler_params=pltpu.CompilerParams(vmem_limit_bytes=LIMIT),
    )(pltpu.with_memory_space_constraint(mixed, pltpu.VMEM), pltpu.with_memory_space_constraint(new_state, pltpu.VMEM))


def solution(mesh):
    in_specs = (
        P(("grp", "tp"), "dp"),
        P(None, ("grp", "dp"), "tp", None, None),
        P(("grp", "dp")),
        P(None, "dp"),
        P(None, "dp", "tp"),
        P(None, "dp", "tp"),
        P(None, "dp", "tp"),
        P(None, "dp", "tp"),
        P(None, "tp", "dp"),
        P(None, "tp"),
        P(None, "tp"),
        P(),
    )
    out_specs = (P(("grp", "tp"), "dp"), P(None, ("grp", "dp"), "tp", None, None))
    body = functools.partial(shards, mesh.shape["tp"], mesh.shape["dp"])
    return jax.shard_map(body, mesh=mesh, in_specs=in_specs, out_specs=out_specs, check_vma=False)
```

```python
import functools

import jax
import jax.numpy as jnp
from jax import lax
from jax.experimental import pallas as pl
from jax.experimental.pallas import tpu as pltpu
from jax.sharding import PartitionSpec as P

LENGTH_MEAN = 512
epsilon = 1e-06
GROUP = 8
PARTS = 4
RELAYS = 2
EARLY = 3
LIMIT = 26 * 1024 * 1024
MESH_ID = pl.DeviceIdType.MESH
f32 = jnp.float32
bf16 = jnp.bfloat16


ORDER = (
    "P0", "P1", "E0", "M0", "E1", "N0", "M1", "N1", "G0", "A0", "P2", "G1", "A1", "P3", "O0", "E2", "M2",
    "Z0", "N2", "E3", "M3", "N3", "G2", "A2", "O1", "Y0", "P4", "Z1", "G3", "A3", "E4", "O2", "Y1", "P5",
    "E5", "M4", "N4", "Z2", "O3", "Z3", "Y2", "P6", "M5", "V1", "N5", "Y3", "P7", "G4", "E6", "E7", "M6",
    "N6", "M7", "N7", "G5", "A4", "G6", "A5", "V3", "A6", "G7", "A7", "V0", "O5", "O4", "O6", "O7", "Y5",
    "V2", "Y6", "Y4", "Y7",
)


def chain(
    n_tp,
    n_dp,
    width,
    parts,
    tokens,
    state,
    lengths,
    gain,
    w_query,
    w_forget,
    w_input,
    w_gate,
    w_out,
    bound,
    pace,
    head_gain,
    mixed,
    sbuf,
    late_forget,
    late_value,
    lengths_s,
    gain_s,
    bound_s,
    pace_s,
    hgain_s,
    forget_s,
    value_s,
    xall,
    wbuf,
    wobuf,
    pf,
    sqx,
    psend,
    precv,
    relay,
    nall,
    po,
    osend,
    orecv,
    pair,
    zsend,
    zrecv,
    gate_s,
    qf_s,
    qk_s,
    ro_s,
    in_sem,
    t_sem,
    w_sem,
    s_sem,
    x_ss,
    x_rs,
    p_ss,
    p_rs,
    r_rs,
    q_ss,
    q_rs,
    n_ss,
    n_rs,
    o_ss,
    o_rs,
    d_ss,
    d_rs,
    z_ss,
    z_rs,
):
    t, d = lax.axis_index("tp"), lax.axis_index("dp")
    rt, feats = tokens.shape
    own, heads, size = state.shape[1], state.shape[2], state.shape[3]
    chans = heads * size
    hr, rh = own // parts, rt // parts
    rows_all = n_dp * hr
    per_part = hr // GROUP
    relayed = n_dp >= 4
    early = min(EARLY, parts) if n_dp == 4 and parts > 1 else 0
    hops = min(RELAYS, n_dp - 2)
    core, chip, chips = lax.rem(t, 2), lax.div(t, 2), n_tp // 2
    at_end = jnp.logical_or(d == 0, d == n_dp - 1)
    merging = jnp.logical_or(d == 1, d == n_dp - 2)

    def tp_peer(k):
        return lax.rem(t + k, n_tp)

    def dp_peer(k):
        return lax.rem(d + k, n_dp)

    def start_all(copies):
        for c in copies:
            c.start()

    token_loads = [
        pltpu.make_async_copy(tokens.at[pl.ds(p * rh, rh)], xall.at[0, p, t], t_sem.at[p]) for p in range(parts)
    ]
    small = [
        pltpu.make_async_copy(src, dst, in_sem.at[i])
        for i, (src, dst) in enumerate(
            ((gain, gain_s), (lengths, lengths_s), (bound, bound_s), (pace, pace_s), (head_gain, hgain_s))
        )
    ]
    loads = []
    for b in range(2):
        per = []
        for i, w in enumerate((w_query, w_forget, w_input, w_gate)):
            per.append(pltpu.make_async_copy(w.at[b], wbuf.at[b, i], w_sem.at[b, i]))
        per.append(pltpu.make_async_copy(w_out.at[b], wobuf.at[b], w_sem.at[b, 4]))
        loads.append(per)

    def state_load(b, g):
        rows = pl.ds(g * GROUP, GROUP)
        return pltpu.make_async_copy(state.at[b, rows], sbuf.at[b, rows], s_sem.at[b, g])

    start_all(token_loads)
    start_all(small)
    start_all(loads[0])

    barrier = pltpu.get_barrier_semaphore()
    for k in range(1, n_tp):
        pl.semaphore_signal(barrier, inc=1, device_id={"tp": tp_peer(k)}, device_id_type=MESH_ID)
    for k in range(1, n_dp):
        pl.semaphore_signal(barrier, inc=1, device_id={"dp": dp_peer(k)}, device_id_type=MESH_ID)
    pl.semaphore_wait(barrier, n_tp + n_dp - 2)

    sends, ready = [], []
    row_id = lax.broadcasted_iota(jnp.int32, (GROUP, size), 0)
    spread = spreader(size)

    def far_first(n):
        return [n // 2] + [k for k in range(1, n) if k != n // 2]

    def x_copy(b, p, k):
        return pltpu.make_async_remote_copy(
            src_ref=xall.at[b, p, t],
            dst_ref=xall.at[b, p, t],
            send_sem=x_ss.at[b, p, k - 1],
            recv_sem=x_rs.at[b, p, k - 1],
            device_id={"tp": tp_peer(k)},
            device_id_type=MESH_ID,
        )

    def share(b, p):
        for k in far_first(n_tp):
            c = x_copy(b, p, k)
            c.start()
            sends.append(c)

    def partial_copy(b, p, k):
        dest = dp_peer(k)
        return pltpu.make_async_remote_copy(
            src_ref=psend.at[b, p, dest],
            dst_ref=precv.at[b, p, k - 1],
            send_sem=p_ss.at[b, p, k - 1],
            recv_sem=p_rs.at[b, p, k - 1],
            device_id={"dp": dest},
            device_id_type=MESH_ID,
        )

    def relay_copy(b, p, k, i):
        return pltpu.make_async_remote_copy(
            src_ref=psend.at[b, p, dp_peer(k)],
            dst_ref=relay.at[b, p, i],
            send_sem=p_ss.at[b, p, k - 1],
            recv_sem=r_rs.at[b, p, i],
            device_id={"dp": jnp.where(d == 0, 1, n_dp - 2)},
            device_id_type=MESH_ID,
        )

    def square_copy(b, p, k):
        return pltpu.make_async_remote_copy(
            src_ref=sqx.at[b, p, d],
            dst_ref=sqx.at[b, p, d],
            send_sem=q_ss.at[b, p, k - 1],
            recv_sem=q_rs.at[b, p, k - 1],
            device_id={"dp": dp_peer(k)},
            device_id_type=MESH_ID,
        )

    def far_along(i):
        middle = far_first(n_dp)[i]
        return jnp.where(d == 0, n_dp - 1 - i, jnp.where(d == n_dp - 1, i + 1, middle))

    def send_partials(b, p):
        for k in range(1, n_dp):
            sends.append(partial_copy(b, p, k))
        if not relayed:
            for k in far_first(n_dp):
                partial_copy(b, p, k).start()
            return

        @pl.when(at_end)
        def _():
            for i in range(n_dp - 2):
                k = jnp.where(d == 0, n_dp - 1 - i, i + 1)
                c = relay_copy(b, p, k, i) if i < hops else partial_copy(b, p, k)
                unless_early(b, p, k, c)

        @pl.when(merging)
        def _():
            for i in range(n_dp - 1 - hops):
                k = jnp.where(d == 1, i, n_dp - i) if i else jnp.where(d == 1, n_dp - 1, 1)
                unless_early(b, p, k, partial_copy(b, p, k))

        if n_dp > 4:

            @pl.when(jnp.logical_not(jnp.logical_or(at_end, merging)))
            def _():
                for k in far_first(n_dp):
                    partial_copy(b, p, k).start()

    def finish_ends(b, p):
        if relayed:

            @pl.when(at_end)
            def _():
                k = jnp.where(d == 0, 1, n_dp - 1)
                unless_early(b, p, k, partial_copy(b, p, k))

    def unless_early(b, p, k, c):
        if b == 0 and p < early:
            pl.when(dp_peer(k) != t)(c.start)
        else:
            c.start()

    def send_early():
        for i in range(4):
            loads[0][i].wait()
        x = jnp.concatenate([xall[0, p, t] for p in range(early)], axis=0).astype(f32)
        gained = (x * gain_s[:1, :].astype(f32)).astype(bf16)
        for i in range(4):
            cols = slice(i * chans, (i + 1) * chans)
            part = jnp.dot(gained, wbuf[0, i], preferred_element_type=f32)
            for p in range(early):
                mine = part[p * hr : (p + 1) * hr]
                pf[p, t, :, cols] = mine
                psend[0, p, t, :, cols] = mine.astype(bf16)
        k = lax.rem(t - d + n_dp, n_dp)

        @pl.when(jnp.logical_and(at_end, t != d))
        def _():
            slot = jnp.where(d == 0, n_dp - 1 - t, t)
            for p in range(early):

                @pl.when(slot < hops)
                def _():
                    relay_copy(0, p, k, slot).start()

                pl.when(slot >= hops)(partial_copy(0, p, k).start)

        @pl.when(jnp.logical_and(merging, t == jnp.where(d == 1, 0, n_dp - 1)))
        def _():
            for p in range(early):
                partial_copy(0, p, k).start()

    def merge(b, p, i):
        @pl.when(merging)
        def _():
            dest = jnp.where(d == 1, n_dp - 1 - i, i)
            k = lax.rem(dest - d + n_dp, n_dp)
            relay_copy(b, p, k, i).wait_recv()
            for j in range(4):
                cols = slice(j * chans, (j + 1) * chans)
                both = pf[p, dest, :, cols] + relay[b, p, i, :, cols].astype(f32)
                psend[b, p, dest, :, cols] = both.astype(bf16)
            partial_copy(b, p, k).start()

    def merge_far(b, p):
        if relayed:
            merge(b, p, 0)

    def merge_near(b, p):
        if relayed:
            for i in range(1, hops):
                merge(b, p, i)

    def bypassed(k):
        source = lax.rem(d - k + n_dp, n_dp)
        low = jnp.logical_and(source == 0, d >= n_dp - hops)
        return jnp.logical_or(low, jnp.logical_and(source == n_dp - 1, d < hops))

    def project(b, p):
        if p == 0 and not (b == 0 and early):
            for i in range(4):
                loads[b][i].wait()
        if b == 0:
            for k in range(1, n_tp):
                x_copy(b, p, k).wait_recv()
        x = xall[b, p].reshape(rows_all, feats).astype(f32)
        sq = jnp.sum(x * x, axis=1, keepdims=True)
        gained = (x * gain_s[b : b + 1, :].astype(f32)).astype(bf16)
        square = lax.broadcasted_iota(jnp.int32, (rows_all, rows_all), 0) == lax.broadcasted_iota(
            jnp.int32, (rows_all, rows_all), 1
        )
        sqx[b, p, d] = jnp.sum(jnp.where(square, sq, 0.0), axis=0, keepdims=True)
        for i in range(n_dp - 1):
            c = square_copy(b, p, far_along(i))
            c.start()
            sends.append(c)
        for i in range(4):
            cols = slice(i * chans, (i + 1) * chans)
            part = jnp.dot(gained, wbuf[b, i], preferred_element_type=f32)
            pf[p, :, :, cols] = part.reshape(n_dp, hr, chans)
            if b == 1 or p >= early:
                psend[b, p, :, :, cols] = part.astype(bf16).reshape(n_dp, hr, chans)
        if b == 0 and p < early:
            for e in range(n_dp):

                @pl.when(t != e)
                def _():
                    psend[0, p, e] = pf[p, e].astype(bf16)

        send_partials(b, p)

    def gates(b, p):
        if b == 0 and p == 0:
            for c in small[1:]:
                c.wait()
        for k in range(1, n_dp):
            c = partial_copy(b, p, k)
            if relayed:
                pl.when(jnp.logical_not(bypassed(k)))(c.wait_recv)
            else:
                c.wait_recv()

        for k in range(1, n_dp):
            square_copy(b, p, k).wait_recv()
        row = sqx[b, p, 0]
        for e in range(1, n_dp):
            row = row + sqx[b, p, e]
        mine = (
            lax.broadcasted_iota(jnp.int32, (hr, rows_all), 1)
            == lax.broadcasted_iota(jnp.int32, (hr, rows_all), 0) + d * hr
        )
        squares = jnp.sum(jnp.where(mine, row, 0.0), axis=1, keepdims=True)
        scale = lax.rsqrt(squares / width + epsilon)

        def total(i):
            cols = slice(i * chans, (i + 1) * chans)
            acc = pf[p, d, :, cols]
            for k in range(n_dp - 1):
                acc = acc + precv[b, p, k, :, cols].astype(f32)
            return scale * acc

        rows = slice(p * hr, (p + 1) * hr)
        log_row = jnp.log(lengths_s[...].astype(f32) / LENGTH_MEAN)
        pick = lax.broadcasted_iota(jnp.int32, (hr, own), 1) == lax.broadcasted_iota(jnp.int32, (hr, own), 0) + p * hr
        log_len = jnp.sum(jnp.where(pick, log_row, 0.0), axis=1, keepdims=True)
        lower = jax.nn.sigmoid(bound_s[b : b + 1, :])
        pre = total(1) - pace_s[b : b + 1, :] * log_len
        forget = lower + (1.0 - lower) * jax.nn.sigmoid(pre)
        key = (1.0 - lower) * jax.nn.sigmoid(-pre)
        if b == 0:
            forget_s[rows] = forget
        else:
            late_forget[rows] = forget
        query = total(0)
        qf_s[...] = query * forget
        qk_s[...] = query * key
        value = value_s if b == 0 else late_value
        value[rows] = total(2)
        gate = total(3)
        gate_s[...] = gate * jax.nn.sigmoid(gate)

        for g in range(per_part):
            state_load(b, p * per_part + g).wait()

        def read(g, carry):
            at = pl.ds(pl.multiple_of(g * GROUP, GROUP), GROUP)
            seqs = pl.ds(pl.multiple_of(p * hr + g * GROUP, GROUP), GROUP)
            for h in range(heads):
                cols = slice(h * size, (h + 1) * size)
                q8 = qf_s[at, cols]
                diag = jnp.concatenate(
                    [jnp.where(row_id == j, q8, 0.0) for j in range(GROUP)], axis=1
                ).astype(bf16)
                s8 = sbuf[b, seqs, h].reshape(GROUP * size, size).astype(bf16)
                ro_s[at, cols] = jnp.dot(diag, s8, preferred_element_type=f32)
            return carry

        lax.fori_loop(0, per_part, read, 0)
        for h in range(heads):
            cols = slice(h * size, (h + 1) * size)
            dots = jnp.sum(qk_s[:, cols], axis=1, keepdims=True)
            readout = ro_s[:, cols] + dots * value[rows, cols]
            mean = jnp.mean(readout * readout, axis=1, keepdims=True)
            normed = readout * lax.rsqrt(mean + epsilon) * hgain_s[b : b + 1, :] * gate_s[:, cols]
            nall[b, p, d, :, cols] = normed.astype(bf16)
    def share_normed(b, p):
        for i in range(n_dp - 1):
            c = normed_copy(b, p, far_along(i))
            c.start()
            sends.append(c)

    def normed_copy(b, p, k):
        return pltpu.make_async_remote_copy(
            src_ref=nall.at[b, p, d],
            dst_ref=nall.at[b, p, d],
            send_sem=n_ss.at[b, p, k - 1],
            recv_sem=n_rs.at[b, p, k - 1],
            device_id={"dp": dp_peer(k)},
            device_id_type=MESH_ID,
        )

    def out_copy(b, p, k):
        dest = tp_peer(k)
        return pltpu.make_async_remote_copy(
            src_ref=osend.at[b, p, dest],
            dst_ref=orecv.at[p, k - 1],
            send_sem=o_ss.at[p, k - 1],
            recv_sem=o_rs.at[p, k - 1],
            device_id={"tp": dest},
            device_id_type=MESH_ID,
        )

    def out_project(b, p):
        if b not in ready:
            ready.append(b)
            loads[b][4].wait()
        for k in range(1, n_dp):
            normed_copy(b, p, k).wait_recv()
        rows = nall[b, p].reshape(rows_all, chans)
        part = jnp.dot(rows, wobuf[b], preferred_element_type=f32)
        po[p] = part.reshape(n_tp, rh, feats)
        osend[b, p] = part.astype(bf16).reshape(n_tp, rh, feats)
        if b == 0:
            c = pair_copy(p)
            c.start()
            sends.append(c)
            return
        for k in far_first(n_tp):
            c = out_copy(b, p, k)
            c.start()
            sends.append(c)

    def pair_copy(p):
        return pltpu.make_async_remote_copy(
            src_ref=osend.at[0, p],
            dst_ref=pair.at[p],
            send_sem=d_ss.at[p],
            recv_sem=d_rs.at[p],
            device_id={"tp": t + 1 - 2 * core},
            device_id_type=MESH_ID,
        )

    def cross_copy(p, i):
        return pltpu.make_async_remote_copy(
            src_ref=zsend.at[p],
            dst_ref=zrecv.at[p, i // 2, core],
            send_sem=z_ss.at[p, i],
            recv_sem=z_rs.at[p, i // 2, core],
            device_id={"tp": lax.rem(2 * chip + i + 2, n_tp)},
            device_id_type=MESH_ID,
        )

    def cross_wait(p, i, c):
        arrived = pltpu.make_async_remote_copy(
            src_ref=zsend.at[p],
            dst_ref=zrecv.at[p, i, c],
            send_sem=z_ss.at[p, i],
            recv_sem=z_rs.at[p, i, c],
            device_id={"tp": lax.rem(t + 1, n_tp)},
            device_id_type=MESH_ID,
        )
        arrived.wait_recv()

    def cross(b, p):
        if b == 1:
            return
        pair_copy(p).wait_recv()
        po[p] = po[p] + pair[p].astype(f32)
        zsend[p] = po[p, pl.ds(core * chips, chips)].astype(bf16)
        for i in range(n_tp - 2):
            c = cross_copy(p, i)
            c.start()
            sends.append(c)

    def residual(b, p):
        if b == 0:
            for c in range(2):
                half = slice(c * chips, (c + 1) * chips)
                branch = po[p, half]
                for i in range(chips - 1):
                    cross_wait(p, i, c)
                    branch = branch + zrecv[p, i, c].astype(f32)
                xall[1, p, half] = (xall[0, p, half].astype(f32) + branch).astype(bf16)
            return
        for k in range(1, n_tp):
            out_copy(b, p, k).wait_recv()
        branch = po[p, t]
        for k in range(n_tp - 1):
            branch = branch + orecv[p, k].astype(f32)
        mixed[p * rh : (p + 1) * rh, :] = xall[b, p, t].astype(f32) + branch

    def advance(b, p):
        def step(g, carry):
            base = pl.multiple_of(p * hr + g * GROUP, GROUP)
            rows = pl.ds(base, GROUP)

            def write(j, h, new):
                sbuf[0, base + j, h] = new

            update(lambda j, h: sbuf[0, base + j, h], write, heads, forget_s[rows, :], value_s[rows, :], spread)
            return carry

        if b == 0:
            lax.fori_loop(0, per_part, step, 0)

    if relayed:
        for k in range(1, n_dp):

            @pl.when(bypassed(k))
            def _():
                for b in range(2):
                    for p in range(parts):
                        precv[b, p, k - 1] = jnp.zeros(precv.shape[3:], bf16)

    for p in range(parts):
        token_loads[p].wait()
        share(0, p)
    for g in range(own // GROUP):
        state_load(0, g).start()
    start_all(loads[1])
    for g in range(own // GROUP):
        state_load(1, g).start()
    small[0].wait()
    if early:
        send_early()

    if parts == 1:
        order = [(f, k) for k in range(2) for f in "PEMNGAVOZY"]
    else:
        order = [(step[0], int(step[1:])) for step in ORDER]
    stages = dict(
        P=project,
        E=finish_ends,
        M=merge_far,
        N=merge_near,
        G=gates,
        A=share_normed,
        O=out_project,
        Z=cross,
        Y=residual,
        V=advance,
    )
    for name, k in order:
        f, b, p = stages[name], k // parts, k % parts
        f(b, p)

    for c in sends:
        c.wait_send()


def spreader(size):
    lane = lax.broadcasted_iota(jnp.int32, (GROUP, GROUP * size), 1)
    row = lax.broadcasted_iota(jnp.int32, (GROUP, GROUP * size), 0)
    ones = jnp.where(lane // size == row, 1.0, 0.0).astype(bf16)
    return jnp.concatenate([ones] * 3, axis=0)


def update(read, write, heads, forget, value, spread):
    size = value.shape[1] // heads
    top = forget.astype(bf16)
    rest = forget - top.astype(f32)
    mid = rest.astype(bf16)
    low = (rest - mid.astype(f32)).astype(bf16)
    pieces = jnp.concatenate([top, mid, low], axis=0)
    for h in range(heads):
        cols = slice(h * size, (h + 1) * size)
        for j in range(0, GROUP, 2):
            wide = lax.dot_general(
                pieces[:, cols],
                spread[:, j * size : (j + 2) * size],
                (((0,), (0,)), ((), ())),
                preferred_element_type=f32,
            )
            for i in range(2):
                row = value[j + i : j + i + 1, cols]
                keep = wide[:, i * size : (i + 1) * size]
                write(j + i, h, row + keep * (read(j + i, h) - row))


def store(mixed, new_state, forget, value, mixed_out, state_out, fresh, sems):
    own, heads, size = new_state.shape[1:4]
    groups = own // GROUP

    def early(g):
        rows = pl.ds(g * GROUP, GROUP)
        return pltpu.make_async_copy(new_state.at[0, rows], state_out.at[0, rows], sems.at[0, g])

    def late(g):
        rows = pl.ds(g * GROUP, GROUP)
        return pltpu.make_async_copy(fresh.at[rows], state_out.at[1, rows], sems.at[1, g])

    rest = pltpu.make_async_copy(mixed, mixed_out, sems.at[2, 0])
    rest.start()
    for g in range(groups):
        early(g).start()
    spread = spreader(size)

    def step(g, carry):
        base = pl.multiple_of(g * GROUP, GROUP)
        rows = pl.ds(base, GROUP)

        def write(j, h, new):
            fresh[base + j, h] = new

        update(lambda j, h: new_state[1, base + j, h], write, heads, forget[rows, :], value[rows, :], spread)
        late(g).start()
        return carry

    lax.fori_loop(0, groups, step, 0)
    rest.wait()
    for g in range(groups):
        early(g).wait()
        late(g).wait()


def shards(n_tp, n_dp, tokens, state, lengths, gain, w_query, w_forget, w_input, w_gate, w_out, bound, pace, head_gain):
    rt, feats = tokens.shape
    own, heads, size = state.shape[1:4]
    chans = heads * size
    parts = PARTS if own == rt and own % (2 * GROUP * PARTS) == 0 else 1
    hr, rh = own // parts, rt // parts
    msg = 4 * chans
    vmem = pl.BlockSpec(memory_space=pltpu.VMEM)
    hbm = pl.BlockSpec(memory_space=pl.ANY)
    dma = pltpu.SemaphoreType.DMA
    late = pltpu.VMEM((own, chans), f32)
    outputs = pl.pallas_call(
        functools.partial(chain, n_tp, n_dp, feats * n_dp, parts),
        name="chain",
        out_shape=(pltpu.VMEM((rt, feats), f32), pltpu.VMEM(state.shape, f32), late, late),
        in_specs=[hbm] * 12,
        out_specs=(vmem,) * 4,
        scratch_shapes=[
            pltpu.VMEM((1, own), jnp.int32),
            pltpu.VMEM(gain.shape, bf16),
            pltpu.VMEM(bound.shape, f32),
            pltpu.VMEM(pace.shape, f32),
            pltpu.VMEM(head_gain.shape, f32),
            pltpu.VMEM((own, chans), f32),
            pltpu.VMEM((own, chans), f32),
            pltpu.VMEM((2, parts, n_tp, rh, feats), bf16),
            pltpu.VMEM((2, 4, feats, chans), bf16),
            pltpu.VMEM((2, chans, feats), bf16),
            pltpu.VMEM((parts, n_dp, hr, 4 * chans), f32),
            pltpu.VMEM((2, parts, n_dp, 1, n_dp * hr), f32),
            pltpu.VMEM((2, parts, n_dp, hr, msg), bf16),
            pltpu.VMEM((2, parts, n_dp - 1, hr, msg), bf16),
            pltpu.VMEM((2, parts, max(n_dp - 2, 1), hr, msg), bf16),
            pltpu.VMEM((2, parts, n_dp, hr, chans), bf16),
            pltpu.VMEM((parts, n_tp, rh, feats), f32),
            pltpu.VMEM((2, parts, n_tp, rh, feats), bf16),
            pltpu.VMEM((parts, n_tp - 1, rh, feats), bf16),
            pltpu.VMEM((parts, n_tp, rh, feats), bf16),
            pltpu.VMEM((parts, n_tp // 2, rh, feats), bf16),
            pltpu.VMEM((parts, n_tp // 2 - 1, 2, n_tp // 2, rh, feats), bf16),
            pltpu.VMEM((hr, chans), f32),
            pltpu.VMEM((hr, chans), f32),
            pltpu.VMEM((hr, chans), f32),
            pltpu.VMEM((hr, chans), f32),
            dma((5,)),
            dma((parts,)),
            dma((2, 5)),
            dma((2, own // GROUP)),
            dma((2, parts, n_tp - 1)),
            dma((2, parts, n_tp - 1)),
            dma((2, parts, n_dp - 1)),
            dma((2, parts, n_dp - 1)),
            dma((2, parts, max(n_dp - 2, 1))),
            dma((2, parts, n_dp - 1)),
            dma((2, parts, n_dp - 1)),
            dma((2, parts, n_dp - 1)),
            dma((2, parts, n_dp - 1)),
            dma((parts, n_tp - 1)),
            dma((parts, n_tp - 1)),
            dma((parts,)),
            dma((parts,)),
            dma((parts, n_tp - 2)),
            dma((parts, n_tp // 2 - 1, 2)),
        ],
        compiler_params=pltpu.CompilerParams(
            collective_id=0, has_side_effects=True, vmem_limit_bytes=LIMIT
        ),
    )(tokens, state, lengths[None, :], gain, w_query, w_forget, w_input, w_gate, w_out, bound, pace, head_gain)

    return pl.pallas_call(
        store,
        name="store",
        out_shape=(jax.ShapeDtypeStruct((rt, feats), f32), jax.ShapeDtypeStruct(state.shape, f32)),
        in_specs=[vmem] * 4,
        out_specs=(hbm, hbm),
        scratch_shapes=[pltpu.VMEM(state.shape[1:], f32), dma((3, own // GROUP))],
        compiler_params=pltpu.CompilerParams(vmem_limit_bytes=LIMIT),
    )(*(pltpu.with_memory_space_constraint(x, pltpu.VMEM) for x in outputs))


def solution(mesh):
    in_specs = (
        P(("grp", "tp"), "dp"),
        P(None, ("grp", "dp"), "tp", None, None),
        P(("grp", "dp")),
        P(None, "dp"),
        P(None, "dp", "tp"),
        P(None, "dp", "tp"),
        P(None, "dp", "tp"),
        P(None, "dp", "tp"),
        P(None, "tp", "dp"),
        P(None, "tp"),
        P(None, "tp"),
        P(),
    )
    out_specs = (P(("grp", "tp"), "dp"), P(None, ("grp", "dp"), "tp", None, None))
    body = functools.partial(shards, mesh.shape["tp"], mesh.shape["dp"])
    return jax.shard_map(body, mesh=mesh, in_specs=in_specs, out_specs=out_specs, check_vma=False)
```
